32 devices in a mesh: sp: 8 (over z, x), tp: 4 (over y, core).
Axes of the slice: x: 2, y: 2, z: 4, core: 2. Of those that a mesh axis runs over, the one named last changes fastest.
Arguments:
- tokens: bfloat16 [4096, 2048], P(('sp', 'tp')), may hold values from -8 to 8
- in_gain: float32 [2048], replicated, may hold values from 0.1 to 1.9
- w_conv_val: bfloat16 [2048, 1024], P('sp', 'tp'), may hold values from -0.125 to 0.125
- w_conv_gate: bfloat16 [2048, 1024], P('sp', 'tp'), may hold values from -0.125 to 0.125
- w_query: bfloat16 [2048, 1024], P('sp', 'tp'), may hold values from -1 to 1
- w_key: bfloat16 [2048, 256], P('sp', 'tp'), may hold values from -1 to 1
- value_weight: bfloat16 [2048, 256], P('sp', 'tp'), may hold values from -0.125 to 0.125
- conv_taps: float32 [31, 1024], P(None, 'tp'), may hold values from -1 to 1
- conv_bias: float32 [1024], P('tp'), may hold values from -3 to 3
- norm_gain: float32 [1024], P('tp'), may hold values from 0.1 to 1.9
- norm_bias: float32 [1024], P('tp'), may hold values from -3 to 3
- head_sink_logit: float32 [16], P('tp'), may hold values from 4 to 7
- w_out_conv: bfloat16 [1024, 2048], P('tp', 'sp'), may hold values from -0.125 to 0.125
- w_out_attn: bfloat16 [1024, 2048], P('tp', 'sp'), may hold values from -0.125 to 0.125
Outputs:
- mixed: bfloat16 [4096, 2048], P(('sp', 'tp'))
- log_total: float32 [4096, 16], P('sp', 'tp')
The draws below stay inside these ranges and needn't reach their ends.
All inputs are finite; a program needn't handle non-finite values.
Results may differ from the reference program's by a relative error of at most 0.012.
Values may be sent and summed in bfloat16 or wider, within the bound.
No kernel may reach another device: no remote copies, remote signals or barrier semaphores. Data moves between devices by JAX's collectives and lax.ppermute only.
A program may use at most 64 MiB of HBM per device.

```python
import math
import jax
import jax.numpy as jnp
from jax import lax

MODEL_WIDTH = 2048
CONV = 1024
QUERY_HEADS = 16
KEY_VALUE_HEADS = 4
HEAD_WIDTH = 64
CONV_TAPS = 31
WINDOW_REACH = 128
TOK_DEV = 512
TOKENS = 4096


def planted_parts(key):
    random_seed_key = jax.random.fold_in(key, 101)
    direction = jnp.where(jax.random.bernoulli(jax.random.fold_in(random_seed_key, 1), 0.5, (MODEL_WIDTH,)), 1.0, -1.0).astype(jnp.float32)
    mask_pattern = jnp.where(jax.random.bernoulli(jax.random.fold_in(random_seed_key, 2), 0.5, (KEY_VALUE_HEADS, HEAD_WIDTH)), 1.0, -1.0).astype(jnp.float32)
    strength = math.sqrt(288.0) / HEAD_WIDTH ** 0.25
    return (direction, mask_pattern, strength)


def draw_tokens(key, part):
    direction, mask_pattern, strength = planted_parts(key)
    jitter = jnp.clip(jax.random.normal(jax.random.fold_in(key, 201), (TOKENS, MODEL_WIDTH), jnp.float32), -4.0, 4.0)
    levels = jnp.exp(jax.random.uniform(jax.random.fold_in(key, 202), (TOKENS, 1), jnp.float32, math.log(0.7), math.log(4.0)))
    chosen = jax.random.bernoulli(jax.random.fold_in(key, 203), 0.125, (TOKENS, 1))
    result = jnp.where(chosen, levels * direction[None, :] + jitter, jitter)
    return result.astype(jnp.bfloat16)


def draw_w_query(key, part):
    direction, mask_pattern, strength = planted_parts(key)
    random_draws = jnp.clip(jax.random.normal(jax.random.fold_in(key, 301), (MODEL_WIDTH, QUERY_HEADS * HEAD_WIDTH), jnp.float32), -4.0, 4.0) * MODEL_WIDTH ** (-0.5)
    column_list = jnp.repeat(mask_pattern, QUERY_HEADS // KEY_VALUE_HEADS, axis=0).reshape(QUERY_HEADS * HEAD_WIDTH)
    result = random_draws + strength / MODEL_WIDTH * direction[:, None] * column_list[None, :]
    return result.astype(jnp.bfloat16)


def draw_w_key(key, part):
    direction, mask_pattern, strength = planted_parts(key)
    random_draws = jnp.clip(jax.random.normal(jax.random.fold_in(key, 401), (MODEL_WIDTH, KEY_VALUE_HEADS * HEAD_WIDTH), jnp.float32), -4.0, 4.0) * MODEL_WIDTH ** (-0.5)
    column_list = mask_pattern.reshape(KEY_VALUE_HEADS * HEAD_WIDTH)
    result = random_draws + strength / MODEL_WIDTH * direction[:, None] * column_list[None, :]
    return result.astype(jnp.bfloat16)


def shard_levels(own_key, dims, split, smallest, high):
    def one(dim, parts):
        steps = jax.random.uniform(jax.random.fold_in(jax.random.fold_in(own_key, 6), dim), (parts,), jnp.float32, smallest / len(split), high / len(split))
        return jnp.repeat(jnp.exp(steps), dims[dim] // parts).reshape((-1,) + (1,) * (len(dims) - dim - 1))

    factor_of = one(*split[0])
    for cut in split[1:]:
        factor_of = factor_of * one(*cut)
    return factor_of


def centred(key, extent, scale, most, shards=(), held_as=jnp.bfloat16):
    entries = scale * jax.random.normal(key, extent, jnp.float32)
    if shards:
        entries = entries * shard_levels(key, extent, shards, -0.22, 0.18)
    return jnp.clip(entries, -most, most).astype(held_as)


def setup_inputs(seed: int = 0) -> dict:
    splits = jax.random.split(jax.random.key(seed), 15)
    return {
        "tokens": draw_tokens(jax.random.fold_in(splits[14], 71), 0),
        "in_gain": jnp.clip(1.0 + 0.18 * jax.random.normal(splits[1], (MODEL_WIDTH,), jnp.float32), 0.1, 1.9),
        "w_conv_val": centred(splits[2], (MODEL_WIDTH, CONV), MODEL_WIDTH ** -0.5, 0.125, ((0, 8), (1, 4))),
        "w_conv_gate": centred(splits[3], (MODEL_WIDTH, CONV), MODEL_WIDTH ** -0.5, 0.125, ((0, 8), (1, 4))),
        "w_query": draw_w_query(jax.random.fold_in(splits[14], 71), 0),
        "w_key": draw_w_key(jax.random.fold_in(splits[14], 71), 0),
        "value_weight": centred(splits[6], (MODEL_WIDTH, KEY_VALUE_HEADS * HEAD_WIDTH), MODEL_WIDTH ** -0.5, 0.125, ((0, 8), (1, 4))),
        "conv_taps": centred(splits[7], (CONV_TAPS, CONV), CONV_TAPS ** -0.5, 1.0, ((1, 4),), jnp.float32),
        "conv_bias": centred(splits[8], (CONV,), 0.5, 3.0, ((0, 4),), jnp.float32),
        "norm_gain": jnp.clip(1.0 + 0.18 * jax.random.normal(splits[9], (CONV,), jnp.float32), 0.1, 1.9),
        "norm_bias": centred(splits[10], (CONV,), 0.5, 3.0, ((0, 4),), jnp.float32),
        "head_sink_logit": jnp.clip(4.0 + 3.0 * jax.random.uniform(splits[11], (QUERY_HEADS,), jnp.float32) ** shard_levels(splits[11], (QUERY_HEADS,), ((0, 4),), -0.2, 0.2), 4.0, 7.0),
        "w_out_conv": centred(splits[12], (CONV, MODEL_WIDTH), (CONV + QUERY_HEADS * HEAD_WIDTH) ** -0.5, 0.125, ((0, 4), (1, 8))),
        "w_out_attn": centred(splits[13], (QUERY_HEADS * HEAD_WIDTH, MODEL_WIDTH), (CONV + QUERY_HEADS * HEAD_WIDTH) ** -0.5, 0.125, ((0, 4), (1, 8))),
    }


def reference(tokens, in_gain, w_conv_val, w_conv_gate, w_query, w_key, value_weight, conv_taps, conv_bias, norm_gain, norm_bias, head_sink_logit, w_out_conv, w_out_attn):
    every_row = tokens.shape[0]
    flt = tokens.astype(jnp.float32)
    normed = (flt * lax.rsqrt(lax.optimization_barrier(jnp.mean(flt * flt, axis=-1, keepdims=True)) + 1e-06) * in_gain).astype(jnp.bfloat16)
    val_part = jnp.dot(normed, w_conv_val, preferred_element_type=jnp.float32)
    gate_part = jnp.dot(normed, w_conv_gate, preferred_element_type=jnp.float32)
    glu = (val_part * jax.nn.sigmoid(gate_part)).astype(jnp.bfloat16)
    half = CONV_TAPS // 2
    padded = jnp.pad(glu, ((half, half), (0, 0)))
    filtered = jnp.zeros(glu.shape, jnp.float32) + conv_bias
    for offset in range(CONV_TAPS):
        filtered = filtered + padded[offset:offset + every_row].astype(jnp.float32) * conv_taps[offset]
    center = lax.optimization_barrier(jnp.mean(filtered, axis=-1, keepdims=True))
    spread = lax.optimization_barrier(jnp.mean((filtered - center) ** 2, axis=-1, keepdims=True))
    conv_out = jax.nn.silu((filtered - center) * lax.rsqrt(spread + 1e-05) * norm_gain + norm_bias).astype(jnp.bfloat16)
    query_matrix = jnp.dot(normed, w_query, preferred_element_type=jnp.float32).astype(jnp.bfloat16)
    key = jnp.dot(normed, w_key, preferred_element_type=jnp.float32).astype(jnp.bfloat16)
    value_matrix = jnp.dot(normed, value_weight, preferred_element_type=jnp.float32).astype(jnp.bfloat16)
    query_groups = QUERY_HEADS // KEY_VALUE_HEADS
    query4_grouped = query_matrix.reshape(every_row, KEY_VALUE_HEADS, query_groups, HEAD_WIDTH)
    padded_keys = jnp.pad(key.reshape(every_row, KEY_VALUE_HEADS, HEAD_WIDTH), ((WINDOW_REACH, WINDOW_REACH), (0, 0), (0, 0)))
    padded_values = jnp.pad(value_matrix.reshape(every_row, KEY_VALUE_HEADS, HEAD_WIDTH), ((WINDOW_REACH, WINDOW_REACH), (0, 0), (0, 0)))
    block = TOK_DEV
    sink_column = head_sink_logit.reshape(KEY_VALUE_HEADS, query_groups, 1)

    def attend(index):
        first = (index * block).astype(jnp.int32)
        qblock = lax.dynamic_slice_in_dim(query4_grouped, first, block, 0).astype(jnp.float32)
        kblock = lax.dynamic_slice_in_dim(padded_keys, first, block + 2 * WINDOW_REACH, 0).astype(jnp.float32)
        vblock = lax.dynamic_slice_in_dim(padded_values, first, block + 2 * WINDOW_REACH, 0).astype(jnp.float32)
        scores = jnp.einsum('qkgd,jkd->kgqj', qblock, kblock) * HEAD_WIDTH ** (-0.5)
        qpos = first + jnp.arange(block, dtype=jnp.int32)
        kpos = first - WINDOW_REACH + jnp.arange(block + 2 * WINDOW_REACH, dtype=jnp.int32)
        valid = (jnp.abs(qpos[:, None] - kpos[None, :]) <= WINDOW_REACH) & (kpos[None, :] >= 0) & (kpos[None, :] < every_row)
        masked = jnp.where(valid, scores, -1e+30)
        top = jnp.maximum(lax.optimization_barrier(jnp.max(masked, axis=-1)), sink_column)
        expd = jnp.where(valid, jnp.exp(masked - top[..., None]), 0.0)
        total = lax.optimization_barrier(jnp.sum(expd, axis=-1)) + jnp.exp(sink_column - top)
        probs = (expd / total[..., None]).astype(jnp.bfloat16)
        attended = jnp.einsum('kgqj,jkd->qkgd', probs.astype(jnp.float32), vblock).astype(jnp.bfloat16)
        log_block = (top + jnp.log(total)).reshape(QUERY_HEADS, block).T
        return (attended.reshape(block, QUERY_HEADS * HEAD_WIDTH), log_block)
    attended, log_total = lax.map(attend, jnp.arange(every_row // block, dtype=jnp.int32))
    attended = attended.reshape(every_row, QUERY_HEADS * HEAD_WIDTH)
    log_total = log_total.reshape(every_row, QUERY_HEADS)
    features = jnp.concatenate([conv_out, attended], axis=1)
    weights_all = jnp.concatenate([w_out_conv, w_out_attn], axis=0)
    mixed = jnp.dot(features, weights_all, preferred_element_type=jnp.float32).astype(jnp.bfloat16)
    return (mixed, log_total)
```

```python
import jax
import jax.numpy as jnp
from jax import lax
from jax.sharding import PartitionSpec as P

WINDOW_REACH = 128
RING_LIMIT = 16


def snake(count):
    return list(range(0, count, 2)) + list(range(count - 1 - count % 2, 0, -2))


def ring_steps(order, step):
    count = len(order)
    return [(order[i], order[(i + step) % count]) for i in range(count)]


def ring_gather(up, down, axis, order):
    ups, downs = [up], [down]
    for _ in range(len(order) - 1):
        up = lax.ppermute(up, axis, ring_steps(order, 1))
        down = lax.ppermute(down, axis, ring_steps(order, -1))
        ups.append(up)
        downs.append(down)
    return ups + downs


def blocks_of(cells, count, dim):
    width = cells.shape[dim] // count
    return [lax.slice_in_dim(cells, i * width, (i + 1) * width, axis=dim) for i in range(count)]


def arrival_columns(cells, order, axis):
    count = len(order)
    place = jnp.asarray([order.index(i) for i in range(count)], jnp.int32)[lax.axis_index(axis)]
    halves = blocks_of(cells, 2 * count, 1)
    width = halves[0].shape[1]
    up = [halves[2 * order[-i % count]] for i in range(count)]
    down = [halves[2 * order[i] + 1] for i in range(count)]
    ups = jnp.concatenate(up + up, axis=1)
    downs = jnp.concatenate(down + down, axis=1)
    span = count * width
    return jnp.concatenate(
        [
            lax.dynamic_slice_in_dim(ups, ((count - place) % count) * width, span, axis=1),
            lax.dynamic_slice_in_dim(downs, place * width, span, axis=1),
        ],
        axis=1,
    )


def source_columns(cells, order, axis):
    count = len(order)
    place = jnp.asarray([order.index(i) for i in range(count)], jnp.int32)[lax.axis_index(axis)]
    span = cells.shape[1] // 2
    width = span // count
    ups, downs = cells[:, :span], cells[:, span:]
    ups = lax.dynamic_slice_in_dim(
        jnp.concatenate([ups, ups], axis=1), place * width, span, axis=1
    )
    downs = lax.dynamic_slice_in_dim(
        jnp.concatenate([downs, downs], axis=1), ((count - place) % count) * width, span, axis=1
    )
    up, down = blocks_of(ups, count, 1), blocks_of(downs, count, 1)
    pieces = []
    for i in range(count):
        pieces.append(up[-order.index(i) % count])
        pieces.append(down[order.index(i)])
    return jnp.concatenate(pieces, axis=1)


def flips(count, bit):
    return [(i, i ^ bit) for i in range(count)]


def rows_gather(rows, axis):
    count = lax.axis_size(axis)
    here = lax.axis_index(axis)
    bit = count // 2
    held = rows[None]
    while bit:
        other = lax.ppermute(held, axis, flips(count, bit))
        low = (here & bit) == 0
        first, second = jnp.where(low, held, other), jnp.where(low, other, held)
        held = jnp.stack([first, second], axis=1).reshape((-1,) + rows.shape)
        bit //= 2
    return held.reshape((-1,) + rows.shape[1:])


def rows_scatter(parts, axis):
    count = lax.axis_size(axis)
    here = lax.axis_index(axis)
    bit = 1
    held = parts.reshape((count, parts.shape[0] // count) + parts.shape[1:])
    while bit < count:
        low = (here & bit) == 0
        pairs = held.reshape((held.shape[0] // 2, 2) + held.shape[1:])
        mine = jnp.where(low, pairs[:, 0], pairs[:, 1])
        yours = jnp.where(low, pairs[:, 1], pairs[:, 0])
        got = lax.ppermute(yours, axis, flips(count, bit))
        held = (mine.astype(jnp.float32) + got.astype(jnp.float32)).astype(parts.dtype)
        bit *= 2
    return held[0]


def small_sum(cells, axis):
    count = lax.axis_size(axis)
    total = cells
    for step in range(1, count):
        total = total + lax.ppermute(cells, axis, [(i, (i + step) % count) for i in range(count)])
    return total


def halo(cells, width, dim):
    count = lax.axis_size("sp")
    ends = count - 1
    head = lax.slice_in_dim(cells, 0, width, axis=dim)
    tail = lax.slice_in_dim(cells, cells.shape[dim] - width, cells.shape[dim], axis=dim)
    return jnp.concatenate(
        [
            lax.ppermute(tail, "sp", [(i, i + 1) for i in range(ends)]),
            cells,
            lax.ppermute(head, "sp", [(i + 1, i) for i in range(ends)]),
        ],
        axis=dim,
    )


def on_device(
    tokens,
    in_gain,
    w_conv_val,
    w_conv_gate,
    w_query,
    w_key,
    value_weight,
    conv_taps,
    conv_bias,
    norm_gain,
    norm_bias,
    head_sink_logit,
    w_out_conv,
    w_out_attn,
):
    spc = lax.axis_size("sp")
    tpc = lax.axis_size("tp")
    ring = spc <= RING_LIMIT
    order = snake(spc)
    flt = tokens.astype(jnp.float32)
    normed = (
        flt * lax.rsqrt(jnp.mean(flt * flt, axis=-1, keepdims=True) + 1e-06) * in_gain
    ).astype(jnp.bfloat16)
    if ring:
        normed = arrival_columns(normed, order, "sp")
    if tpc & (tpc - 1) == 0:
        rows = rows_gather(normed, "tp")
    else:
        rows = lax.all_gather(normed, "tp", axis=0, tiled=True)
    chans = w_conv_val.shape[1]
    qwidth = w_query.shape[1]
    kwidth = w_key.shape[1]

    def project(weights):
        if ring:
            top, bottom = blocks_of(weights, 2, 0)
            full = jnp.concatenate(ring_gather(top, bottom, "sp", order), axis=0)
        else:
            full = lax.all_gather(weights, "sp", axis=0, tiled=True)
        return jnp.dot(rows, full, preferred_element_type=jnp.float32)

    attn_in = project(jnp.concatenate([w_query, w_key, value_weight], axis=1))
    conv_in = project(jnp.concatenate([w_conv_val, w_conv_gate], axis=1))
    out_here = jnp.concatenate([w_out_conv, w_out_attn], axis=0)
    if ring:
        left, right = blocks_of(out_here, 2, 1)
        out_rows = jnp.concatenate(ring_gather(left, right, "sp", order), axis=1)
    else:
        out_rows = lax.all_gather(out_here, "sp", axis=1, tiled=True)

    length = rows.shape[0]
    glu = (conv_in[:, :chans] * jax.nn.sigmoid(conv_in[:, chans:])).astype(jnp.bfloat16)
    query_matrix = attn_in[:, :qwidth].astype(jnp.bfloat16)
    keys_values = attn_in[:, qwidth:].astype(jnp.bfloat16)

    heads_here = head_sink_logit.shape[0]
    head_size = qwidth // heads_here
    kv_here = kwidth // head_size
    query_groups = heads_here // kv_here
    banded = halo(keys_values, WINDOW_REACH, 0)
    span = length + 2 * WINDOW_REACH
    key_band = banded[:, :kwidth].reshape(span, kv_here, head_size)
    value_band = banded[:, kwidth:].reshape(span, kv_here, head_size)
    query4_grouped = query_matrix.reshape(length, kv_here, query_groups, head_size)
    scores = jnp.einsum(
        "qkgd,jkd->kgqj", query4_grouped, key_band, preferred_element_type=jnp.float32
    ) * head_size ** (-0.5)
    offset_pos = lax.axis_index("sp") * length
    seq_len = length * spc
    qpos = offset_pos + jnp.arange(length, dtype=jnp.int32)
    kpos = offset_pos - WINDOW_REACH + jnp.arange(span, dtype=jnp.int32)
    valid = (
        (jnp.abs(qpos[:, None] - kpos[None, :]) <= WINDOW_REACH)
        & (kpos[None, :] >= 0)
        & (kpos[None, :] < seq_len)
    )
    sink_column = head_sink_logit.reshape(kv_here, query_groups, 1)
    masked = jnp.where(valid, scores, -1e30)
    top = jnp.maximum(jnp.max(masked, axis=-1), sink_column)
    expd = jnp.where(valid, jnp.exp(masked - top[..., None]), 0.0)
    total = jnp.sum(expd, axis=-1) + jnp.exp(sink_column - top)
    probs = (expd / total[..., None]).astype(jnp.bfloat16)
    attended = jnp.einsum(
        "kgqj,jkd->qkgd", probs, value_band, preferred_element_type=jnp.float32
    ).astype(jnp.bfloat16)
    attended = attended.reshape(length, qwidth)
    log_total = (top + jnp.log(total)).reshape(heads_here, length).T

    taps = conv_taps.shape[0]
    padded = halo(glu, taps // 2, 0)
    filtered = jnp.zeros(glu.shape, jnp.float32) + conv_bias
    for offset in range(taps):
        filtered = (
            filtered + padded[offset : offset + length].astype(jnp.float32) * conv_taps[offset]
        )
    sums = small_sum(
        jnp.stack([jnp.sum(filtered, axis=-1), jnp.sum(filtered * filtered, axis=-1)]), "tp"
    )
    count = chans * tpc
    center = (sums[0] / count)[:, None]
    spread = (sums[1] / count)[:, None] - center * center
    conv_out = jax.nn.silu(
        (filtered - center) * lax.rsqrt(spread + 1e-05) * norm_gain + norm_bias
    ).astype(jnp.bfloat16)

    features = jnp.concatenate([conv_out, attended], axis=1)
    parts = jnp.dot(features, out_rows, preferred_element_type=jnp.float32).astype(jnp.bfloat16)
    if tpc & (tpc - 1) == 0:
        mixed = rows_scatter(parts, "tp")
    else:
        mixed = lax.psum_scatter(parts, "tp", scatter_dimension=0, tiled=True)
    if ring:
        mixed = source_columns(mixed, order, "sp")
    return (mixed, log_total)


def solution(mesh):
    return jax.shard_map(
        on_device,
        mesh=mesh,
        in_specs=(
            P(("sp", "tp"), None),
            P(),
            P("sp", "tp"),
            P("sp", "tp"),
            P("sp", "tp"),
            P("sp", "tp"),
            P("sp", "tp"),
            P(None, "tp"),
            P("tp"),
            P("tp"),
            P("tp"),
            P("tp"),
            P("tp", "sp"),
            P("tp", "sp"),
        ),
        out_specs=(P(("sp", "tp"), None), P("sp", "tp")),
        check_vma=False,
    )
```
